32 devices in a mesh: grp: 2 (over y), sp: 4 (over z), tp: 4 (over x, core).
Axes of the slice: x: 2, y: 2, z: 4, core: 2. Of those that a mesh axis runs over, the one named last changes fastest.
Arguments:
- tokens: bfloat16 [3072, 2048], P(('grp', 'sp')), parts along dimension 0, may hold values from -6 to 6
- norm_gain: float32 [2, 2048], replicated, may hold values from 0.1 to 1.9
- entry_weight: bfloat16 [2, 2048, 2048], P(None, 'sp', 'tp'), may hold values from -0.125 to 0.125
- mix_weight: bfloat16 [2, 4, 512, 512], P(None, 'tp'), may hold values from -0.25 to 0.25
- pool_gain: float32 [2, 2048], P(None, 'tp'), may hold values from 0.1 to 1.9
- back_weight: bfloat16 [2, 2048, 2048], P(None, 'tp', 'sp'), may hold values from -0.25 to 0.25
Outputs:
- result_tokens: bfloat16 [3072, 2048], P(('grp', 'sp')), parts along dimension 0
The draws below stay inside these ranges and needn't reach their ends.
There are 2 independent parts, one for each index of `grp`. The reference program is written for one: setup_inputs(seed, part) draws one part's arguments, and reference() takes and returns one part's arrays. A program takes and returns all parts, laid end to end along the dimension named above; an argument that names none is the same for every part. Nothing has to cross between parts.
All inputs are finite; a program needn't handle non-finite values.
Results may differ from the reference program's by a relative error of at most 0.018.
Values may be sent and summed in bfloat16 or wider, within the bound.
No kernel may reach another device: no remote copies, remote signals or barrier semaphores. Data moves between devices by JAX's collectives and lax.ppermute only.
A program may use at most 64 MiB of HBM per device.

```python
import jax
import jax.numpy as jnp
from jax import lax

D = 2048
GROUPS = 4
POOL_W = 2048
GROUP_W = 512
LAYERS = 2
LENGTH = 1536
N_TP = 4


def steps_of(own_key, extent, shards, low, largest):
    factor_of = 1.0
    for axis_at, parts in shards:
        heights = jax.random.uniform(jax.random.fold_in(jax.random.fold_in(own_key, 6), axis_at), (parts,), jnp.float32, low / len(shards), largest / len(shards))
        factor_of = factor_of * jnp.repeat(jnp.exp(heights), extent[axis_at] // parts).reshape((-1,) + (1,) * (len(extent) - 1 - axis_at))
    return factor_of


def normal_values(stream_key, dims, width, bound, split=(), held_as=jnp.bfloat16):
    values = jax.random.normal(stream_key, dims, jnp.float32) * width
    if len(split) > 0:
        values = steps_of(stream_key, dims, split, -0.22, 0.18) * values
    return jnp.clip(values, min=-bound, max=bound).astype(held_as)


def setup_inputs(seed: int = 0, part: int = 0) -> dict:
    splits = jax.random.split(jax.random.key(seed), 7)
    part_splits = jax.random.split(jax.random.fold_in(splits[6], part), 7)
    return {
        "tokens": normal_values(part_splits[0], (LENGTH, D), 1.0, 6.0, ((0, 4),)),
        "norm_gain": jnp.clip(1.0 + 0.18 * jax.random.normal(splits[1], (LAYERS, D), jnp.float32), 0.1, 1.9),
        "entry_weight": normal_values(splits[2], (LAYERS, D, POOL_W), D ** -0.5, 0.125, ((1, 4), (2, 4))),
        "mix_weight": normal_values(splits[3], (LAYERS, GROUPS, GROUP_W, GROUP_W), GROUP_W ** -0.5, 0.25, ((1, 4),)),
        "pool_gain": jnp.clip(1.0 + 0.18 * jax.random.normal(splits[4], (LAYERS, POOL_W), jnp.float32), 0.1, 1.9),
        "back_weight": normal_values(splits[5], (LAYERS, POOL_W, D), (POOL_W // 4) ** -0.5, 0.25, ((1, 4), (2, 4))),
    }


EPSILON = 1e-05

def window_mean(padded, positions, halves, total_length, reach):
    row_count = positions.shape[0]
    summed = jnp.zeros((row_count,) + padded.shape[1:], jnp.float32)
    for offset in range(-reach, reach):
        inside = ((offset >= -halves) & (offset < halves)).astype(jnp.float32)
        summed = summed + padded[reach + offset:reach + offset + row_count] * inside[None, :, None]
    lower = jnp.maximum(positions[:, None] - halves[None, :], 0)
    upper = jnp.minimum(positions[:, None] + halves[None, :], total_length)
    counted = (upper - lower).astype(jnp.float32)
    return summed / counted[:, :, None]

def reference(tokens, norm_gain, entry_weight, mix_weight, pool_gain, back_weight):
    reach = 2 ** (GROUPS - 1)
    halves = jnp.left_shift(jnp.int32(1), jnp.arange(GROUPS, dtype=jnp.int32))
    positions = jnp.arange(LENGTH, dtype=jnp.int32)
    block_width = POOL_W // N_TP
    state = tokens
    for layer in range(LAYERS):
        values = state.astype(jnp.float32)
        scaled = values * lax.rsqrt(lax.optimization_barrier(jnp.mean(values * values, axis=-1, keepdims=True)) + EPSILON)
        normed = (scaled * norm_gain[layer].astype(jnp.float32)).astype(jnp.bfloat16)
        pooled_in = jnp.dot(normed, entry_weight[layer], preferred_element_type=jnp.float32).astype(jnp.bfloat16)
        grouped = pooled_in.reshape(LENGTH, GROUPS, GROUP_W).astype(jnp.float32)
        padded = jnp.pad(grouped, ((reach, reach), (0, 0), (0, 0)))
        means = window_mean(padded, positions, halves, LENGTH, reach)
        differ = (means - grouped).astype(jnp.bfloat16)
        mixed = jnp.einsum('tgc,gcd->tgd', differ.astype(jnp.float32), mix_weight[layer].astype(jnp.float32))
        mixed = (mixed.reshape(LENGTH, POOL_W) * pool_gain[layer].astype(jnp.float32)).astype(jnp.bfloat16)
        total = values
        for block in range(N_TP):
            term = jnp.dot(mixed[:, block * block_width:(block + 1) * block_width], back_weight[layer, block * block_width:(block + 1) * block_width], preferred_element_type=jnp.float32)
            total = total + lax.optimization_barrier(term.astype(jnp.bfloat16)).astype(jnp.float32)
        state = total.astype(jnp.bfloat16)
    return state
```

```python
import jax
import jax.numpy as jnp
import numpy as np
from jax import lax
from jax.sharding import PartitionSpec as P

GROUPS = 4
LAYERS = 2
EPSILON = 1e-05
RING_MAX = 8
F32 = jnp.float32
BF16 = jnp.bfloat16


def ring_order(count):
    return list(range(0, count, 2)) + list(range(1, count, 2))[::-1]


def dot(a, b):
    return jnp.dot(a, b, preferred_element_type=F32)


class Plan:
    def __init__(self):
        count = lax.axis_size("sp")
        order = ring_order(count)
        self.count = count
        self.succ = [(order[i], order[(i + 1) % count]) for i in range(count)]
        self.pred = [(b, a) for a, b in self.succ]
        self.ahead = count // 2
        self.behind = count - 1 - self.ahead
        offsets = [0]
        for k in range(1, self.ahead + 1):
            offsets.append(-k)
            if k <= self.behind:
                offsets.append(k)
        place = {device: i for i, device in enumerate(order)}
        table = [[order[(place[d] + o) % count] for o in offsets] for d in range(count)]
        inverse = [[row.index(s) for s in range(count)] for row in table]
        here = lax.axis_index("sp")
        self.block = jnp.asarray(np.array(table, np.int32))[here]
        self.inverse = jnp.asarray(np.array(inverse, np.int32))[here]
        self.half = lax.axis_index("grp")
        self.swap = [(0, 1), (1, 0)]

    def gather(self, mine):
        blocks = [mine]
        forward = backward = mine
        for k in range(1, self.ahead + 1):
            forward = lax.ppermute(forward, "sp", self.succ)
            blocks.append(forward)
            if k <= self.behind:
                backward = lax.ppermute(backward, "sp", self.pred)
                blocks.append(backward)
        return blocks

    def halves(self, weight, axis):
        size = weight.shape[axis] // 2
        mine = lax.dynamic_slice_in_dim(weight, self.half * size, size, axis)
        other = lax.dynamic_slice_in_dim(weight, (1 - self.half) * size, size, axis)
        return mine, other

    def all_halves(self, weight, axis):
        mine, other = self.halves(weight, axis)
        first = self.gather(mine)
        second = [other] + [lax.ppermute(b, "grp", self.swap) for b in first[1:]]
        return list(zip(first, second))

    def relative(self, value, axis):
        size = value.shape[axis] // self.count // 2
        parts = []
        for k in range(self.count):
            for h in range(2):
                at = self.block[k] * (2 * size) + ((self.half + h) % 2) * size
                parts.append(lax.dynamic_slice_in_dim(value, at, size, axis))
        return jnp.concatenate(parts, axis)

    def absolute(self, value):
        size = value.shape[1] // self.count // 2
        parts = []
        for s in range(self.count):
            for h in range(2):
                at = self.inverse[s] * (2 * size) + ((self.half + h) % 2) * size
                parts.append(lax.dynamic_slice_in_dim(value, at, size, 1))
        return jnp.concatenate(parts, 1)


def reduce_pairs(mixed, weights, state, members):
    index = lax.axis_index("tp")
    rows = mixed.shape[0]
    low = index % 2
    near = [(i, i ^ 1) for i in range(members)]
    half = rows // 2

    def mul(value):
        return jnp.concatenate([dot(value, w) for w in weights], 1)

    theirs = lax.dynamic_slice_in_dim(mixed, (1 - low) * half, half, 0)
    ours = lax.dynamic_slice_in_dim(mixed, low * half, half, 0)
    got = lax.ppermute(mul(theirs).astype(BF16), "tp", near)
    summed = mul(ours).astype(BF16).astype(F32) + got.astype(F32)
    step = 2
    while step < members:
        sent = summed.astype(BF16)
        got = lax.ppermute(sent, "tp", [(i, i ^ step) for i in range(members)])
        summed = sent.astype(F32) + got.astype(F32)
        step *= 2
    base = lax.dynamic_slice_in_dim(state, low * half, half, 0)
    fresh = (base.astype(F32) + summed).astype(BF16)
    other = lax.ppermute(fresh, "tp", near)
    first = jnp.where(low == 0, fresh, other)
    second = jnp.where(low == 0, other, fresh)
    return jnp.concatenate([first, second], 0)


def ring_device(tokens, norm_gain, entry_weight, mix_weight, pool_gain, back_weight):
    reach = 2 ** (GROUPS - 1)
    plan = Plan()
    rows = tokens.shape[0]
    channels = tokens.shape[1]
    members = lax.axis_size("tp")
    wide = reach * LAYERS
    sp_size = plan.count
    entry, back = [], []
    for layer in range(LAYERS):
        entry.append(plan.all_halves(entry_weight[layer], 0))
        back.append(plan.all_halves(back_weight[layer], 1))
    up = [(i, i + 1) for i in range(sp_size - 1)]
    down = [(j, i) for i, j in up]
    before = lax.ppermute(tokens[rows - wide :], "sp", up)
    after = lax.ppermute(tokens[:wide], "sp", down)
    state = plan.relative(jnp.concatenate([before, tokens, after], 0), 1)
    gains = plan.relative(norm_gain, 1)
    total = sp_size * rows
    window = jnp.left_shift(jnp.int32(1), lax.axis_index("tp"))
    piece = channels // sp_size // 2
    for layer in range(LAYERS):
        margin = reach * (LAYERS - layer)
        start = lax.axis_index("sp") * rows - margin
        count_in = rows + 2 * margin
        count_out = count_in - 2 * reach
        values = state.astype(F32)
        scale = lax.rsqrt(jnp.mean(values * values, axis=-1, keepdims=True) + EPSILON)
        normed = (values * scale * gains[layer]).astype(BF16)
        pooled = 0.0
        for k, pair in enumerate(entry[layer]):
            for h, w in enumerate(pair):
                at = (2 * k + h) * piece
                pooled = pooled + dot(normed[:, at : at + piece], w)
        where_in = start + lax.broadcasted_iota(jnp.int32, (count_in, 1), 0)
        inside = (where_in >= 0) & (where_in < total)
        pooled = jnp.where(inside, pooled, 0.0).astype(BF16)
        r = lax.broadcasted_iota(jnp.int32, (count_out, count_in), 0) + reach
        c = lax.broadcasted_iota(jnp.int32, (count_out, count_in), 1)
        band = ((c >= r - window) & (c < r + window)).astype(BF16)
        summed = dot(band, pooled)
        at = start + reach + lax.broadcasted_iota(jnp.int32, (count_out, 1), 0)
        counted = jnp.minimum(at + window, total) - jnp.maximum(at - window, 0)
        counted = jnp.maximum(counted, 1).astype(F32)
        middle = pooled[reach : reach + count_out].astype(F32)
        differ = (summed / counted - middle).astype(BF16)
        mixed = (dot(differ, mix_weight[layer, 0]) * pool_gain[layer]).astype(BF16)
        old = state[reach : reach + count_out]
        chunks = []
        half = (sp_size + 1) // 2
        for lo, hi in ((0, half), (half, sp_size)):
            weights = [w for pair in back[layer][lo:hi] for w in pair]
            base = old[:, 2 * lo * piece : 2 * hi * piece]
            chunks.append(reduce_pairs(mixed, weights, base, members))
        state = jnp.concatenate(chunks, 1)
    return plan.absolute(state)


def extended_2(value, sides, width):
    for axis, dim in sides:
        size, length = (lax.axis_size(axis), value.shape[dim])
        up = [(i, (i + 1) % size) for i in range(size - 1)]
        down = [(j, i) for i, j in up]
        last = lax.slice_in_dim(value, length - width, length, axis=dim)
        first = lax.slice_in_dim(value, 0, width, axis=dim)
        before = lax.ppermute(last, axis, up)
        after = lax.ppermute(first, axis, down)
        value = jnp.concatenate([before, value, after], axis=dim)
    return value


def window_mean(padded, positions, halves, total_length, reach):
    row_count = positions.shape[0]
    summed = jnp.zeros((row_count,) + padded.shape[1:], jnp.float32)
    for offset in range(-reach, reach):
        inside = ((offset >= -halves) & (offset < halves)).astype(jnp.float32)
        summed = (
            summed + padded[reach + offset : reach + offset + row_count] * inside[None, :, None]
        )
    lower = jnp.maximum(positions[:, None] - halves[None, :], 0)
    upper = jnp.minimum(positions[:, None] + halves[None, :], total_length)
    counted = (upper - lower).astype(jnp.float32)
    return summed / counted[:, :, None]


def normalize(state, gain):
    values = state.astype(jnp.float32)
    scaled = values * lax.rsqrt(jnp.mean(values * values, axis=-1, keepdims=True) + EPSILON)
    return (scaled * gain).astype(jnp.bfloat16)


def pool_groups(pooled_in, mix_layer, gain_layer, reach):
    row_count = pooled_in.shape[0]
    group_here = mix_layer.shape[0]
    width = mix_layer.shape[1]
    extended = extended_2(pooled_in, (("sp", 0),), reach)
    first_group = lax.axis_index("tp") * group_here
    halves = jnp.left_shift(jnp.int32(1), first_group + jnp.arange(group_here, dtype=jnp.int32))
    positions = lax.axis_index("sp") * row_count + jnp.arange(row_count, dtype=jnp.int32)
    total_length = lax.axis_size("sp") * row_count
    padded = extended.reshape(row_count + 2 * reach, group_here, width).astype(jnp.float32)
    means = window_mean(padded, positions, halves, total_length, reach)
    differ = (means - padded[reach : reach + row_count]).astype(jnp.bfloat16)
    mixed = jnp.einsum("tgc,gcd->tgd", differ, mix_layer, preferred_element_type=jnp.float32)
    return (mixed.reshape(row_count, group_here * width) * gain_layer).astype(jnp.bfloat16)


def plain_device(tokens, norm_gain, entry_weight, mix_weight, pool_gain, back_weight):
    reach = 2 ** (GROUPS - 1)
    state = tokens
    entry_all, back_all = (
        lax.all_gather(entry_weight, "sp", axis=1, tiled=True),
        lax.all_gather(back_weight, "sp", axis=2, tiled=True),
    )
    for layer in range(LAYERS):
        normed = normalize(state, norm_gain[layer])
        pooled_in = dot(normed, entry_all[layer]).astype(jnp.bfloat16)
        mixed = pool_groups(pooled_in, mix_weight[layer], pool_gain[layer], reach)
        update = dot(mixed, back_all[layer])
        summed = lax.psum(update.astype(jnp.bfloat16), "tp").astype(jnp.float32)
        state = (state.astype(jnp.float32) + summed).astype(jnp.bfloat16)
    return state


def solution(mesh):
    size = dict(mesh.shape)
    members = size["tp"]
    ring = (
        size["grp"] == 2
        and 2 <= size["sp"] <= RING_MAX
        and members == GROUPS
        and members & (members - 1) == 0
    )
    return jax.shard_map(
        ring_device if ring else plain_device,
        mesh=mesh,
        in_specs=(
            P(("grp", "sp"), None),
            P(),
            P(None, "sp", "tp"),
            P(None, "tp", None, None),
            P(None, "tp"),
            P(None, "tp", "sp"),
        ),
        out_specs=P(("grp", "sp"), None),
        check_vma=False,
    )
```
